32 devices in a mesh: sp: 4 (over y, x), tp: 8 (over z, core).
Axes of the slice: x: 2, y: 2, z: 4, core: 2. Of those that a mesh axis runs over, the one named last changes fastest.
Arguments:
- latent: bfloat16 [4096, 2048], P(('sp', 'tp')), may hold values from -1.5 to 1.5
- context: bfloat16 [128, 2048], P('sp'), may hold values from -6 to 6
- cond: bfloat16 [2048], replicated, may hold values from -6 to 6
- cond_context: bfloat16 [2048], replicated, may hold values from -6 to 6
- mod_weight: bfloat16 [3, 2048, 2048], P(None, 'sp', 'tp'), may hold values from -0.125 to 0.125
- norm_gain: bfloat16 [2048], replicated, may hold values from 0.099609375 to 1.8984375
- down_q: bfloat16 [2048, 768], P('tp'), may hold values from -0.125 to 0.125
- down_kv: bfloat16 [2048, 512], P('tp'), may hold values from -0.125 to 0.125
- rope_weight: bfloat16 [2048, 32], replicated, may hold values from -0.125 to 0.125
- qlat_gain: bfloat16 [768], replicated, may hold values from 0.099609375 to 1.8984375
- kvlat_gain: bfloat16 [512], replicated, may hold values from 0.099609375 to 1.8984375
- up_query: bfloat16 [768, 1536], P(None, 'tp'), may hold values from -0.21875 to 0.21875
- up_key: bfloat16 [512, 1024], P(None, 'tp'), may hold values from -0.25 to 0.25
- up_value: bfloat16 [512, 1024], P(None, 'tp'), may hold values from -0.25 to 0.25
- query_gain: float32 [96], replicated, may hold values from 0.5 to 8
- key_gain: float32 [96], replicated, may hold values from 0.5 to 8
- context_bias: float32 [16], P('tp'), may hold values from -2.2 to -0.7
- out_weight: bfloat16 [1024, 2048], P('tp'), may hold values from -24 to 24
Outputs:
- mixed: bfloat16 [4096, 2048], P(('sp', 'tp'))
The draws below stay inside these ranges and needn't reach their ends.
All inputs are finite; a program needn't handle non-finite values.
Results may differ from the reference program's by a relative error of at most 0.028.
The reference program's roundings to bfloat16 on the way count: a program that leaves them out, or rounds other values in their place, can miss the bound.
Values may be sent and summed in bfloat16 or wider, within the bound.
A program may use at most 64 MiB of HBM per device.

```python
import math
import jax
import jax.numpy as jnp
from jax import lax

D = 2048
HEADS = 16
NOPE = 64
ROPE = 32
VDIM = 64
QRANK = 768
KVRANK = 512
GRID_W = 64
TOK_DEV = 1024
CTX_DEV = 32
TOKENS = 4096
CONTEXT = 128


def draw_gain_vector(key):
    return jax.random.uniform(key, (NOPE + ROPE,), jnp.float32, 1.1, 1.9)


def draw_query_gain(key, part):
    return draw_gain_vector(jax.random.fold_in(key, 11))


def draw_key_gain(key, part):
    return draw_gain_vector(jax.random.fold_in(key, 23))


def level_of(own_key, shape, cuts, smallest, largest):
    level = 1.0
    for position, blocks in cuts:
        heights = jax.random.uniform(jax.random.fold_in(jax.random.fold_in(own_key, 6), position), (blocks,), jnp.float32, smallest / len(cuts), largest / len(cuts))
        level = level * jnp.repeat(jnp.exp(heights), shape[position] // blocks).reshape((-1,) + (1,) * (len(shape) - 1 - position))
    return level


def bell_draw(own_key, shape, deviation, bound, cuts=(), held_as=jnp.bfloat16):
    level = level_of(own_key, shape, cuts, -0.22, 0.18) if cuts else 1.0
    result = jax.random.normal(own_key, shape, jnp.float32) * deviation * level
    return jnp.minimum(jnp.maximum(result, -bound), bound).astype(held_as)


def setup_inputs(seed: int = 0) -> dict:
    streams_of = jax.random.split(jax.random.key(seed), 19)
    latent = bell_draw(streams_of[0], (TOKENS, D), 0.25, 1.5, ((0, 32),))
    context = bell_draw(streams_of[1], (CONTEXT, D), 1.0, 6.0, ((0, 4),))
    cond = bell_draw(streams_of[2], (D,), 1.0, 6.0)
    cond_context = bell_draw(streams_of[3], (D,), 1.0, 6.0)
    mod_weight = bell_draw(streams_of[4], (3, D, D), D ** -0.5, 0.125, ((1, 4), (2, 8)))
    norm_gain = jnp.clip(1.0 + 0.18 * jax.random.normal(streams_of[5], (D,), jnp.float32), 0.099609375, 1.8984375).astype(jnp.bfloat16)
    down_q = bell_draw(streams_of[6], (D, QRANK), D ** -0.5, 0.125, ((0, 8),))
    down_kv = bell_draw(streams_of[7], (D, KVRANK), D ** -0.5, 0.125, ((0, 8),))
    rope_weight = bell_draw(streams_of[8], (D, ROPE), D ** -0.5, 0.125)
    qlat_gain = jnp.clip(1.0 + 0.18 * jax.random.normal(streams_of[9], (QRANK,), jnp.float32), 0.099609375, 1.8984375).astype(jnp.bfloat16)
    kvlat_gain = jnp.clip(1.0 + 0.18 * jax.random.normal(streams_of[10], (KVRANK,), jnp.float32), 0.099609375, 1.8984375).astype(jnp.bfloat16)
    up_query = bell_draw(streams_of[11], (QRANK, HEADS * (NOPE + ROPE)), QRANK ** -0.5, 0.21875, ((1, 8),))
    up_key = bell_draw(streams_of[12], (KVRANK, HEADS * NOPE), KVRANK ** -0.5, 0.25, ((1, 8),))
    up_value = bell_draw(streams_of[13], (KVRANK, HEADS * VDIM), KVRANK ** -0.5, 0.25, ((1, 8),))
    query_gain = draw_query_gain(jax.random.fold_in(streams_of[18], 71), 0)
    key_gain = draw_key_gain(jax.random.fold_in(streams_of[18], 71), 0)
    context_bias = jnp.clip(-2.2 + 1.5 * jax.random.uniform(streams_of[16], (HEADS,), jnp.float32) ** level_of(streams_of[16], (HEADS,), ((0, 8),), -0.2, 0.2), -2.2, -0.7)
    out_weight = bell_draw(streams_of[17], (HEADS * VDIM, D), (2.0 * (TOKENS + CONTEXT) ** 0.5 * (HEADS * VDIM) ** -0.5), 24.0, ((0, 8),))
    return dict(latent=latent, context=context, cond=cond, cond_context=cond_context, mod_weight=mod_weight, norm_gain=norm_gain, down_q=down_q, down_kv=down_kv, rope_weight=rope_weight, qlat_gain=qlat_gain, kvlat_gain=kvlat_gain, up_query=up_query, up_key=up_key, up_value=up_value, query_gain=query_gain, key_gain=key_gain, context_bias=context_bias, out_weight=out_weight)


epsilon = 1e-06
theta = 10000.0

def rounded(tensor):
    return lax.optimization_barrier(tensor.astype(jnp.bfloat16))

def rms_scale(tensor, gain):
    return tensor * lax.rsqrt(lax.optimization_barrier(jnp.mean(tensor * tensor, axis=-1, keepdims=True)) + epsilon) * gain.astype(jnp.float32)

def axial_tables(positions):
    pair_count = ROPE // 4
    frequency = jnp.power(theta, -jnp.arange(pair_count, dtype=jnp.float32) / pair_count)
    row_angle = (positions // GRID_W).astype(jnp.float32)[:, None] * frequency
    col_angle = (positions % GRID_W).astype(jnp.float32)[:, None] * frequency
    return (jnp.cos(row_angle), jnp.sin(row_angle), jnp.cos(col_angle), jnp.sin(col_angle))

def rotate_half(tensor, cosine, sine_table):
    first, second = jnp.split(tensor, 2, axis=-1)
    cosine = cosine[:, None, :]
    sine_table = sine_table[:, None, :]
    return jnp.concatenate([first * cosine - second * sine_table, second * cosine + first * sine_table], axis=-1)

def axial_rotate(tensor, tables):
    half_width = tensor.shape[-1] // 2
    return jnp.concatenate([rotate_half(tensor[..., :half_width], tables[0], tables[1]), rotate_half(tensor[..., half_width:], tables[2], tables[3])], axis=-1)

def modulate(row_block, gain, shifts, scales):
    normal = rms_scale(row_block.astype(jnp.float32), gain)
    return rounded(normal * (1.0 + scales) + shifts)

def make_queries(query_latent, up_query, query_gain, tables):
    amount = query_latent.shape[0]
    projected = jnp.dot(query_latent, up_query, preferred_element_type=jnp.float32).reshape(amount, -1, NOPE + ROPE)
    normal = rms_scale(projected, query_gain)
    return rounded(jnp.concatenate([normal[..., :NOPE], axial_rotate(normal[..., NOPE:], tables)], axis=-1))

def make_keys(kv_latent, rope_rows, up_key, up_value, key_gain, tables):
    amount = kv_latent.shape[0]
    unrotated = jnp.dot(kv_latent, up_key, preferred_element_type=jnp.float32).reshape(amount, -1, NOPE)
    head_count = unrotated.shape[1]
    shared = jnp.broadcast_to(rope_rows.astype(jnp.float32)[:, None, :], (amount, head_count, ROPE))
    normal = rms_scale(jnp.concatenate([unrotated, shared], axis=-1), key_gain)
    if tables is not None:
        normal = jnp.concatenate([normal[..., :NOPE], axial_rotate(normal[..., NOPE:], tables)], axis=-1)
    values = jnp.dot(kv_latent, up_value, preferred_element_type=jnp.float32).reshape(amount, head_count, VDIM)
    return (rounded(normal), rounded(values))

def attend(query_block, keys, values, context_keys, context_values, context_shift):
    scaling = (NOPE + ROPE) ** (-0.5)
    query_wide = query_block.astype(jnp.float32)
    latent_scores = jnp.einsum('qhd,khd->qhk', query_wide, keys.astype(jnp.float32)) * scaling
    context_scores = jnp.einsum('qhd,khd->qhk', query_wide, context_keys.astype(jnp.float32)) * scaling
    context_scores = context_scores + context_shift[None, :, None]
    row_max = jnp.maximum(lax.optimization_barrier(jnp.max(latent_scores, axis=-1)), lax.optimization_barrier(jnp.max(context_scores, axis=-1)))[..., None]
    latent_weights = jnp.exp(latent_scores - row_max)
    context_weights = jnp.exp(context_scores - row_max)
    totals = lax.optimization_barrier(jnp.sum(latent_weights, axis=-1)) + lax.optimization_barrier(jnp.sum(context_weights, axis=-1))
    summed = jnp.einsum('qhk,khd->qhd', rounded(latent_weights).astype(jnp.float32), values.astype(jnp.float32))
    summed = summed + jnp.einsum('qhk,khd->qhd', rounded(context_weights).astype(jnp.float32), context_values.astype(jnp.float32))
    return rounded(summed / totals[..., None])

def reference(latent, context, cond, cond_context, mod_weight, norm_gain, down_q, down_kv, rope_weight, qlat_gain, kvlat_gain, up_query, up_key, up_value, query_gain, key_gain, context_bias, out_weight):
    activated = rounded(jax.nn.silu(jnp.stack([cond, cond_context]).astype(jnp.float32)))
    shifts, scales, gates = (jnp.dot(activated[0], mod_weight[member], preferred_element_type=jnp.float32) for member in range(3))
    context_shift, context_scale = (jnp.dot(activated[1], mod_weight[member], preferred_element_type=jnp.float32) for member in range(2))
    normed = modulate(latent, norm_gain, shifts, scales)
    context_normed = modulate(context, norm_gain, context_shift, context_scale)
    query_latent = rounded(rms_scale(jnp.dot(normed, down_q, preferred_element_type=jnp.float32), qlat_gain))
    kv_latent = rounded(rms_scale(jnp.dot(normed, down_kv, preferred_element_type=jnp.float32), kvlat_gain))
    context_kv = rounded(rms_scale(jnp.dot(context_normed, down_kv, preferred_element_type=jnp.float32), kvlat_gain))
    rope_rows = rounded(jnp.dot(normed, rope_weight, preferred_element_type=jnp.float32))
    context_rope = rounded(jnp.dot(context_normed, rope_weight, preferred_element_type=jnp.float32))
    tables = axial_tables(jnp.arange(TOKENS, dtype=jnp.int32))
    queries = make_queries(query_latent, up_query, query_gain, tables)
    keys, values = make_keys(kv_latent, rope_rows, up_key, up_value, key_gain, tables)
    context_keys, context_values = make_keys(context_kv, context_rope, up_key, up_value, key_gain, None)
    context_shift_heads = context_bias.astype(jnp.float32) + math.log(TOK_DEV / CTX_DEV)
    block_rows = math.gcd(TOKENS, 256)
    query_blocks = queries.reshape(TOKENS // block_rows, block_rows, HEADS, NOPE + ROPE)
    attended = lax.map(lambda blocks: attend(blocks, keys, values, context_keys, context_values, context_shift_heads), query_blocks)
    attended = attended.reshape(TOKENS, HEADS * VDIM)
    projected = jnp.dot(attended, out_weight, preferred_element_type=jnp.float32)
    return (latent.astype(jnp.float32) + gates * projected).astype(jnp.bfloat16)
```

```python
import math

import jax
import jax.numpy as jnp
import numpy as np
from jax import lax
from jax.experimental import pallas as pl
from jax.experimental.pallas import tpu as pltpu
from jax.sharding import PartitionSpec as P

NOPE = 64
ROPE = 32
VDIM = 64
GRID_W = 64
TOK_DEV = 1024
CTX_DEV = 32
CORES = 2
KD = NOPE + ROPE
WIDE = KD + VDIM

epsilon = 1e-06
theta = 10000.0

NT = (((1,), (1,)), ((), ()))
TN = (((0,), (0,)), ((), ()))
TT = (((0,), (1,)), ((), ()))


def axial_tables(count):
    pair_count = ROPE // 4
    positions = np.arange(count)
    frequency = np.power(theta, -np.arange(pair_count, dtype=np.float32) / pair_count).astype(np.float32)
    row_angle = (positions // GRID_W).astype(np.float32)[None, :] * frequency[:, None]
    col_angle = (positions % GRID_W).astype(np.float32)[None, :] * frequency[:, None]
    tables = [np.cos(row_angle), np.sin(row_angle), np.cos(col_angle), np.sin(col_angle)]
    return np.stack(tables).astype(np.float32)


def remote(source, target, send, recv, device):
    return pltpu.make_async_remote_copy(
        src_ref=source,
        dst_ref=target,
        send_sem=send,
        recv_sem=recv,
        device_id=device,
        device_id_type=pl.DeviceIdType.MESH,
    )


def loop(low, high, body):
    def step(k, carry):
        body(k)
        return carry

    lax.fori_loop(low, high, step, 0)


class Here:
    def __init__(self):
        self.sp, self.tp = lax.axis_index("sp"), lax.axis_index("tp")
        self.S, self.T = lax.axis_size("sp"), lax.axis_size("tp")
        self.X = math.isqrt(self.S)
        assert self.X * self.X == self.S
        self.y, self.x = self.sp // self.X, lax.rem(self.sp, self.X)
        self.Z = self.T // CORES
        self.z, self.core = self.tp // CORES, lax.rem(self.tp, CORES)
        self.mate = {"tp": self.tp + 1 - 2 * self.core}

    def greet(self):
        barrier = pltpu.get_barrier_semaphore()
        for k in range(1, self.S):
            to = lax.rem(self.sp + k, self.S)
            pl.semaphore_signal(barrier, inc=1, device_id={"sp": to}, device_id_type=pl.DeviceIdType.MESH)
        for k in range(1, self.T):
            to = lax.rem(self.tp + k, self.T)
            pl.semaphore_signal(barrier, inc=1, device_id={"tp": to}, device_id_type=pl.DeviceIdType.MESH)
        pl.semaphore_wait(barrier, self.S + self.T - 2)

    def block(self, r):
        z, Z = self.z, self.Z
        near = lax.min(z, Z - 1 - z)
        zig = ((r + 1) // 2) * (2 * lax.rem(r, 2) - 1)
        far = (r - near) * jnp.where(z <= Z - 1 - z, 1, -1)
        return z + jnp.where(r <= 2 * near, zig, far)

    def part(self, dy, dx):
        X = self.X
        return lax.rem(self.y + dy + X, X) * X + lax.rem(self.x + dx + X, X)


class Line:
    def __init__(self, at, own, slot, send, recv):
        self.at, self.own, self.slot, self.send, self.recv = at, own, slot, send, recv

    def hop(self, block, step, first=False):
        at = self.at
        to = lax.max(lax.min(at.z + step, at.Z - 1), 0)
        return remote(
            self.own if first else self.slot(block),
            self.slot(block),
            self.send.at[block, (1 - step) // 2],
            self.recv.at[block],
            {"tp": to * CORES + at.core},
        )

    def ends(self, step):
        return (self.at.z + step >= 0) & (self.at.z + step < self.at.Z)

    def start(self):
        for step in (1, -1):

            @pl.when(self.ends(step))
            def _():
                self.hop(self.at.z, step, True).start()

    def way(self, block):
        return jnp.where(block < self.at.z, 1, -1)

    def arrive(self, block):
        step = self.way(block)
        self.hop(block, step).wait_recv()

        @pl.when(self.ends(step))
        def _():
            self.hop(block, step).start()

    def drain(self):
        for step in (1, -1):

            @pl.when(self.ends(step))
            def _():
                self.hop(self.at.z, step, True).wait_send()

        def body(r):
            block = self.at.block(r)
            step = self.way(block)

            @pl.when(self.ends(step))
            def _():
                self.hop(block, step).wait_send()

        loop(1, self.at.Z, body)


class Plane:
    def __init__(self, at, slot, send, recv):
        self.at, self.slot, self.send, self.recv = at, slot, send, recv

    def side(self, b):
        return lax.rem(b + self.at.core, 2)

    def place(self, e, i, j):
        return self.at.part(i * e + j * (1 - e), i * (1 - e) + j * e)

    def copy(self, b, s, to, sem):
        return remote(self.slot(b, s), self.slot(b, s), self.send.at[b, sem], self.recv.at[b, s], {"sp": to})

    def sends(self, b, first, second, act):
        X, e = self.at.X, self.side(b)
        if first:
            for i in range(1, X):
                act(self.copy(b, self.at.sp, self.place(e, i, 0), i - 1))
            for j in range(1, X):
                act(self.copy(b, self.at.sp, self.place(e, 0, j), X + j - 2))
        if second:
            for i in range(1, X):
                for j in range(1, X):
                    sem = 2 * (X - 1) + (i - 1) * (X - 1) + j - 1
                    act(self.copy(b, self.place(e, -i, 0), self.place(e, 0, j), sem))

    def push(self, b):
        self.sends(b, True, False, lambda copy: copy.start())

    def take(self, b, s):
        self.copy(b, s, self.place(0, 1, 0), 0).wait_recv()

    def forward(self, b, then=None):
        e = self.side(b)
        for i in range(1, self.at.X):
            s = self.place(e, -i, 0)
            self.take(b, s)
            if then is not None:
                then(b, s)
        self.sends(b, False, True, lambda copy: copy.start())

    def rest(self, b):
        e = self.side(b)
        for j in range(1, self.at.X):
            for i in range(self.at.X):
                self.take(b, self.place(e, -i, -j))

    def drain(self, b):
        self.sends(b, True, True, lambda copy: copy.wait_send())


class Mate:
    def __init__(self, at, slot, send, recv):
        self.at, self.slot, self.send, self.recv = at, slot, send, recv

    def copy(self, core, *key):
        return remote(self.slot(core, *key), self.slot(core, *key), self.send.at[key], self.recv.at[key], self.at.mate)

    def give(self, *key):
        self.copy(self.at.core, *key).start()

    def take(self, *key):
        self.copy(1 - self.at.core, *key).wait_recv()

    def drain(self, *key):
        self.copy(self.at.core, *key).wait_send()


def rms(tensor, axis):
    return tensor * lax.rsqrt(jnp.mean(tensor * tensor, axis=axis, keepdims=True) + epsilon)


def kernel(
    vectors, gain_q, gain_k, shift,
    latent, context, mod_weight, dq, dkv, ow, rope_w, uq, uk, uv, tables_in,
    out,
    lat, con, mw, rope, up_q, up_k, up_v, tables, uq_t, ukv_t,
    dq_all, dkv_all, ow_all, pm, msum, mods, normed,
    kv_lats, q_lats, ctx_lats, q, kv, ctx_kv, m_scr, l_scr, acc, att, att_in,
    local, p_send, p_recv, t_send, t_recv,
    wl_send, wl_recv, wp_send, wp_recv, wm_send, wm_recv,
    ll_send, ll_recv, lp_send, lp_recv, lm_send, lm_recv, qm_send, qm_recv,
    x_send, x_recv, a_send, a_recv,
):
    at = Here()
    sp, tp, S, T, Z, z, core = at.sp, at.tp, at.S, at.T, at.Z, at.z, at.core
    f32, bf16 = jnp.float32, jnp.bfloat16
    H, N, _ = q.shape
    rows = out.shape[0]
    span = rows * CORES
    ctx_rows = con.shape[0]
    rank = uk.shape[0]
    width = latent.shape[1]
    TQ = span
    factor = KD ** (-0.5) * math.log2(math.e)

    loads = [
        pltpu.make_async_copy(a, b, local.at[i])
        for i, (a, b) in enumerate((
            (mod_weight, mw), (latent, lat), (context, con), (rope_w, rope), (uq, up_q), (uk, up_k), (uv, up_v),
            (tables_in, tables), (dq, dq_all.at[z, core]), (dkv, dkv_all.at[z, core]), (ow, ow_all.at[z, core]),
        ))
    ]
    for copy in loads:
        copy.start()
    at.greet()

    weights = ((dq, dq_all), (dkv, dkv_all), (ow, ow_all))
    w_lines, w_planes, w_mates = [], [], []
    for i, (own, every) in enumerate(weights):
        w_lines.append(Line(
            at, own.at[sp], (lambda e: lambda b: e.at[b, core, sp])(every), wl_send.at[i], wl_recv.at[i]
        ))
        w_planes.append(Plane(at, (lambda e: lambda b, s: e.at[b, core, s])(every), wp_send.at[i], wp_recv.at[i]))
        w_mates.append(Mate(at, (lambda e: lambda c, b: e.at[b, c])(every), wm_send.at[i], wm_recv.at[i]))

    def own_mate(i):
        own, every = weights[i]
        return remote(own, every.at[z, core], wm_send.at[i, z], wm_recv.at[i, z], at.mate)

    for i in range(2):
        w_lines[i].start()

    span_k = mw.shape[1]

    def silu(v):
        return v / (1.0 + jnp.exp(-v))

    where = pl.ds(pl.multiple_of(sp * span_k, span_k), span_k)
    wide = [jnp.broadcast_to(silu(vectors[i : i + 1, where]), (8, span_k)) for i in range(2)]
    index = lax.broadcasted_iota(jnp.int32, (8, span_k), 0)
    loads[0].wait()
    part = jnp.zeros(pm.shape[1:], f32)
    for r in range(mw.shape[0]):
        act = jnp.where(index == 2 * r, wide[0], jnp.where(index == 2 * r + 1, wide[1], 0.0)).astype(bf16)
        part = part + jnp.dot(act, mw[r], preferred_element_type=f32)
    pm[sp] = part

    def part_copy(k):
        return remote(pm.at[sp], pm.at[sp], p_send.at[k], p_recv.at[k], {"sp": lax.rem(sp + k, S)})

    def part_wait(k):
        to = pm.at[lax.rem(sp - k + S, S)]
        remote(to, to, p_send.at[k], p_recv.at[k], {"sp": lax.rem(sp + k, S)}).wait_recv()

    def mod_copy(k):
        return remote(msum, mods.at[tp], t_send.at[k], t_recv.at[k], {"tp": lax.rem(tp + k, T)})

    def mod_wait(k):
        to = mods.at[lax.rem(tp - k + T, T)]
        remote(to, to, t_send.at[k], t_recv.at[k], {"tp": lax.rem(tp + k, T)}).wait_recv()

    loop(1, S, lambda k: part_copy(k).start())
    for i in range(2):
        own_mate(i).start()
    loop(1, S, part_wait)
    total = pm[0]
    for k in range(1, S):
        total = total + pm[k]
    msum[...] = total
    mods[tp] = total
    loop(1, T, lambda k: mod_copy(k).start())

    def weights_arrive(r):
        b = at.block(r)
        for i in range(2):
            w_lines[i].arrive(b)
            w_planes[i].push(b)

    def weights_forward(r):
        b = at.block(r)
        for i in range(2):
            w_planes[i].forward(b)

    for r in range(1, Z):
        weights_arrive(r)
        if r > 1:
            weights_forward(r - 1)
    w_lines[2].start()
    weights_forward(Z - 1)

    for copy in loads[4:7]:
        copy.wait()
    uq_t[...] = up_q[...].astype(f32).T.astype(bf16)
    ukv_t[: H * NOPE, :] = up_k[...].astype(f32).T.astype(bf16)
    ukv_t[H * NOPE :, :] = up_v[...].astype(f32).T.astype(bf16)

    loop(1, T, mod_wait)
    loads[1].wait()
    loads[2].wait()
    gain = vectors[2:3, :]
    every_mod = jnp.concatenate([mods[t] for t in range(T)], axis=1)

    def modulate(source, count, base, kind):
        step = math.gcd(count, 32)
        for i in range(count // step):
            u = source[i * step : (i + 1) * step, :].astype(f32)
            u = rms(u, 1) * gain * (1.0 + every_mod[2 + kind : 3 + kind, :]) + every_mod[kind : kind + 1, :]
            normed[base + i * step : base + (i + 1) * step, :] = u.astype(bf16)

    modulate(lat, rows, 0, 0)
    modulate(con, ctx_rows, rows, 1)

    for r in range(1, Z):
        b = at.block(r)
        w_lines[2].arrive(b)
        for i in range(2):
            w_planes[i].rest(b)
            w_mates[i].give(b)
    for copy in loads[3:4] + loads[7:11]:
        copy.wait()
    for i in range(2):
        for b in range(Z):
            w_mates[i].take(b)

    def tail(u, count):
        u = jnp.concatenate([u, jnp.zeros((count, 128 - ROPE), f32)], axis=1)
        u = jnp.concatenate([u, jnp.zeros((128 - count, 128), f32)], axis=0) if count < 128 else u
        return u.T[:ROPE, :].astype(bf16)

    def put_tail(ref, t):
        ref[-16:, 0:128] = t[:16, :]
        ref[-16:, 128:256] = t[16:, :]

    def get_tail(block, count):
        return jnp.concatenate([block[-16:, 0:128], block[-16:, 128:256]], axis=0)[:, :count]

    stacked = normed[...]
    kv_down = jnp.dot(stacked, dkv_all[...].reshape(width, -1), preferred_element_type=f32)
    kv_latent = (rms(kv_down, 1) * vectors[4:5, :rank]).astype(bf16)
    rope_rows = jnp.dot(stacked, rope[...], preferred_element_type=f32)
    own_kv = kv_lats.at[sp, z, core]
    own_kv[:rows, :] = kv_latent[:rows]
    put_tail(own_kv, tail(rope_rows[:rows], rows))
    own_ctx = ctx_lats.at[sp]
    own_ctx[:ctx_rows, :] = kv_latent[rows:]
    put_tail(own_ctx, tail(rope_rows[rows:], ctx_rows))

    kv_line = Line(at, own_kv, lambda b: kv_lats.at[sp, b, core], ll_send.at[0], ll_recv.at[0])
    kv_plane = Plane(at, lambda b, s: kv_lats.at[s, b, core], lp_send, lp_recv)
    kv_mate = Mate(at, lambda c, s, b: kv_lats.at[s, b, c], lm_send, lm_recv)
    q_line = Line(at, q_lats.at[z, core], lambda b: q_lats.at[b, core], ll_send.at[1], ll_recv.at[1])
    q_mate = Mate(at, lambda c, b: q_lats.at[b, c], qm_send, qm_recv)

    kv_line.start()
    kv_plane.push(z)
    kv_mate.give(sp, z)

    def ctx_copy(k):
        return remote(own_ctx, own_ctx, x_send.at[k], x_recv.at[k], {"sp": lax.rem(sp + k, S)})

    def ctx_wait(k):
        to = ctx_lats.at[lax.rem(sp - k + S, S)]
        remote(to, to, x_send.at[k], x_recv.at[k], {"sp": lax.rem(sp + k, S)}).wait_recv()

    loop(1, S, lambda k: ctx_copy(k).start())

    query_down = jnp.dot(normed[:rows, :], dq_all[...].reshape(width, -1), preferred_element_type=f32)
    q_lats[z, core] = (rms(query_down, 1) * vectors[3:4, : query_down.shape[1]]).astype(bf16)
    q_line.start()
    q_mate.give(z)

    def turned(u, gain, where):
        u = rms(u, 0) * gain[:, :1]
        if where is None:
            return u
        m = ROPE // 4
        a, b, c, d = (u[NOPE + i * m : NOPE + (i + 1) * m, :] for i in range(4))
        rc, rs, cc, cs = (tables[i, :, where] for i in range(4))
        return jnp.concatenate(
            [u[:NOPE, :], a * rc - b * rs, b * rc + a * rs, c * cc - d * cs, d * cc + c * cs], axis=0
        )

    def expand(rows_in, tail_in, to, columns, where):
        u = lax.dot_general(ukv_t[...], rows_in, NT, preferred_element_type=f32)
        for h in range(H):
            key = turned(
                jnp.concatenate([u[h * NOPE : (h + 1) * NOPE, :], tail_in.astype(f32)], axis=0), gain_k[...], where
            )
            to[h * WIDE : h * WIDE + KD, columns] = key.astype(bf16)
            base = H * NOPE + h * VDIM
            to[h * WIDE + KD : (h + 1) * WIDE, columns] = u[base : base + VDIM, :].astype(bf16)

    def kv_forward(r):
        kv_plane.forward(at.block(r), lambda b, s: kv_mate.give(s, b))

    for r in range(1, Z):
        b = at.block(r)
        kv_line.arrive(b)
        kv_plane.push(b)
        kv_mate.give(sp, b)
        kv_forward(r - 1)
    kv_forward(Z - 1)
    for r in range(1, Z):
        w_planes[2].push(at.block(r))
    own_mate(2).start()

    loop(1, S, ctx_wait)
    ctx_block = [ctx_lats[s] for s in range(S)]
    expand(
        jnp.concatenate([block[:ctx_rows, :] for block in ctx_block], axis=0),
        jnp.concatenate([get_tail(block, ctx_rows) for block in ctx_block], axis=1),
        ctx_kv, slice(None), None,
    )

    def chunk(c):
        return at.part(-(c // at.X), -lax.rem(c, at.X))

    def chunk_arrive(c):
        s = chunk(c)

        def body(b):
            e = kv_plane.side(b)
            late = jnp.where(e == 0, c // at.X, lax.rem(c, at.X))

            @pl.when(late != 0)
            def _():
                kv_plane.take(b, s)
                kv_mate.give(s, b)

        loop(0, Z, body)

    def chunk_expand(c):
        s = chunk(c)

        def body(b):
            kv_mate.take(s, b)
            blocks = [kv_lats[s, b, i] for i in range(CORES)]
            expand(
                jnp.concatenate([block[:rows, :] for block in blocks], axis=0),
                jnp.concatenate([get_tail(block, rows) for block in blocks], axis=1),
                kv.at[s],
                pl.ds(pl.multiple_of(b * span, span), span),
                pl.ds(pl.multiple_of(s * N + b * span, span), span),
            )

        loop(0, Z, body)

    def tile_arrive(t):
        b = at.block(t)
        q_line.arrive(b)
        q_mate.give(b)

    def tile_at(t):
        return pl.ds(pl.multiple_of(at.block(t) * TQ, TQ), TQ)

    def lanes(p):
        total = p[:, :128]
        for j in range(1, p.shape[1] // 128):
            total = total + p[:, j * 128 : (j + 1) * 128]
        return total

    def tile_expand(t):
        b = at.block(t)
        q_mate.take(b)
        where = tile_at(t)
        rows_in = q_lats[b].reshape(span, q_lats.shape[3])
        u = lax.dot_general(uq_t[...], rows_in, NT, preferred_element_type=f32)
        for h in range(H):
            spot = pl.ds(pl.multiple_of(sp * N + b * span, span), span)
            query = turned(u[h * KD : (h + 1) * KD, :], gain_q[...], spot)
            query = jnp.concatenate([query, jnp.zeros((128 - KD, span), f32)], axis=0)
            q[h, where, :] = query.T.astype(bf16)
            kt = ctx_kv[h * WIDE : h * WIDE + KD, :]
            vt = ctx_kv[h * WIDE + KD : (h + 1) * WIDE, :]
            s = jnp.dot(q[h, where, :][:, :KD], kt, preferred_element_type=f32) * factor + shift[h : h + 1, :1]
            new = jnp.max(s, axis=1, keepdims=True)
            p = jnp.exp2(s - new)
            m_scr[h, where, :] = jnp.broadcast_to(new, (TQ, 128))
            l_scr[h, where, :] = lanes(p)
            acc[h, where, :] = lax.dot_general(p.astype(bf16), vt, NT, preferred_element_type=f32)

    def pair(t, c):
        where = tile_at(t)
        s_from = chunk(c)
        for h in range(H):
            kt = kv[s_from, h * WIDE : h * WIDE + KD, :]
            vt = kv[s_from, h * WIDE + KD : (h + 1) * WIDE, :]
            s = jnp.dot(q[h, where, :][:, :KD], kt, preferred_element_type=f32) * factor
            old = m_scr[h, where, :][:, :1]
            new = jnp.maximum(old, jnp.max(s, axis=1, keepdims=True))
            scale = jnp.exp2(old - new)
            p = jnp.exp2(s - new)
            m_scr[h, where, :] = jnp.broadcast_to(new, (TQ, 128))
            l_scr[h, where, :] = l_scr[h, where, :] * scale + lanes(p)
            acc[h, where, :] = acc[h, where, :] * scale + lax.dot_general(
                p.astype(bf16), vt, NT, preferred_element_type=f32
            )

    def owner_rows(dest):
        return att.at[pl.ds(pl.multiple_of(dest * rows, rows), rows)]

    def give(dest):
        return remote(owner_rows(dest), att_in.at[tp], a_send.at[dest], a_recv.at[tp], {"tp": dest})

    def finish(t):
        where = tile_at(t)
        heads = [acc[h, where, :] / jnp.sum(l_scr[h, where, :], axis=1, keepdims=True) for h in range(H)]
        att[where, :] = jnp.concatenate(heads, axis=1).astype(bf16)
        for i in range(CORES):
            dest = at.block(t) * CORES + i

            @pl.when(dest != tp)
            def _():
                give(dest).start()

            @pl.when(dest == tp)
            def _():
                att_in[tp] = owner_rows(tp)[...]


    def diagonal(w):
        @pl.when(w < S)
        def _():
            chunk_expand(w)

        @pl.when(w < Z)
        def _():
            tile_expand(w)

        low, high = lax.max(w - S + 1, 0), lax.min(w, Z - 1) + 1

        def one(t):
            pair(t, w - t)

            @pl.when(w - t == S - 1)
            def _():
                finish(t)

        loop(low, high, one)

        @pl.when(w + 1 < S)
        def _():
            chunk_arrive(w + 1)

        @pl.when(w + 1 < Z)
        def _():
            tile_arrive(w + 1)

        @pl.when(w == S - 1)
        def _():
            loop(1, Z, lambda r: w_planes[2].forward(at.block(r)))

    loop(0, Z + S - 1, diagonal)

    def ow_rest(r):
        b = at.block(r)
        w_planes[2].rest(b)
        w_mates[2].give(b)

    loop(1, Z, ow_rest)
    loop(0, Z, lambda b: w_mates[2].take(b))

    def att_wait(k):
        source = lax.rem(tp - k + T, T)
        to = att_in.at[source]
        remote(to, to, a_send.at[source], a_recv.at[source], {"tp": source}).wait_recv()

    loop(1, T, att_wait)
    attended = jnp.concatenate([att_in[t] for t in range(T)], axis=1)
    cut = mods.shape[2]
    for t in range(T):
        where = slice(t * cut, (t + 1) * cut)
        weight = ow_all[:, :, :, :, where].reshape(-1, cut)
        projected = jnp.dot(attended, weight, preferred_element_type=f32)
        out[:, where] = (lat[:, where].astype(f32) + mods[t, 4:5, :] * projected).astype(bf16)

    loop(1, S, lambda k: part_copy(k).wait_send())
    loop(1, T, lambda k: mod_copy(k).wait_send())
    loop(1, S, lambda k: ctx_copy(k).wait_send())
    loop(1, T, lambda k: give(lax.rem(tp + k, T)).wait_send())
    for i in range(3):
        own_mate(i).wait_send()
        w_lines[i].drain()

        def body(r):
            w_planes[i].drain(at.block(r))
            w_mates[i].drain(at.block(r))

        loop(1, Z, body)
    kv_line.drain()
    q_line.drain()

    def body(b):
        kv_plane.drain(b)
        q_mate.drain(b)
        loop(0, S, lambda s: kv_mate.drain(s, b))

    loop(0, Z, body)


DMA = pltpu.SemaphoreType.DMA
VM = pl.BlockSpec(memory_space=pltpu.VMEM)
ANY = pl.BlockSpec(memory_space=pl.ANY)


def shards(
    latent, context, cond, cond_context, mod_weight, norm_gain, down_q, down_kv, rope_weight, qlat_gain, kvlat_gain,
    up_query, up_key, up_value, query_gain, key_gain, context_bias, out_weight,
):
    S, T = lax.axis_size("sp"), lax.axis_size("tp")
    Z = T // CORES
    bf16, f32 = jnp.bfloat16, jnp.float32
    own_rows, width = latent.shape
    ctx_rows = context.shape[0]
    N = own_rows * T
    cols = mod_weight.shape[2]
    dq, dkv, ow = (w.reshape(S, w.shape[0] // S, w.shape[1]) for w in (down_q, down_kv, out_weight))
    QR, KR = down_q.shape[1], down_kv.shape[1]
    H = up_key.shape[1] // NOPE

    def row(v):
        return jnp.pad(v.astype(f32), (0, width - v.shape[0]))[None, :]

    vectors = jnp.concatenate(
        [row(v) for v in (cond, cond_context, norm_gain, qlat_gain, kvlat_gain)] + [jnp.zeros((3, width), f32)], axis=0
    )
    gain_q = jnp.broadcast_to(query_gain[:, None], (KD, 128))
    gain_k = jnp.broadcast_to(key_gain[:, None], (KD, 128))
    shift = (context_bias + math.log(TOK_DEV / CTX_DEV)) * math.log2(math.e)
    shift = jnp.broadcast_to(shift[:, None], (H, 128))
    tables = jnp.asarray(axial_tables(S * N))
    args = (
        vectors, gain_q, gain_k, shift, latent, context, mod_weight, dq, dkv, ow, rope_weight,
        up_query, up_key, up_value, tables,
    )
    lat_rows, kv_rows = own_rows + 16, H * WIDE
    V = pltpu.VMEM
    scratch = [
        V(latent.shape, bf16), V(context.shape, bf16), V(mod_weight.shape, bf16), V(rope_weight.shape, bf16),
        V(up_query.shape, bf16), V(up_key.shape, bf16), V(up_value.shape, bf16), V(tables.shape, f32),
        V(up_query.shape[::-1], bf16), V((H * (NOPE + VDIM), KR), bf16),
        V((Z, CORES) + dq.shape, bf16), V((Z, CORES) + dkv.shape, bf16), V((Z, CORES) + ow.shape, bf16),
        V((S, 8, cols), f32), V((8, cols), f32), V((T, 8, cols), f32), V((own_rows + ctx_rows, width), bf16),
        V((S, Z, CORES, lat_rows, KR), bf16), V((Z, CORES, own_rows, QR), bf16), V((S, ctx_rows + 16, KR), bf16),
        V((H, N, 128), bf16), V((S, kv_rows, N), bf16), V((kv_rows, S * ctx_rows), bf16),
        V((H, N, 128), f32), V((H, N, 128), f32), V((H, N, VDIM), f32),
        V((N, H * VDIM), bf16), V((T, own_rows, H * VDIM), bf16),
        DMA((11,)), DMA((S,)), DMA((S,)), DMA((T,)), DMA((T,)),
        DMA((3, Z, 2)), DMA((3, Z)), DMA((3, Z, S - 1)), DMA((3, Z, S)), DMA((3, Z)), DMA((3, Z)),
        DMA((2, Z, 2)), DMA((2, Z)), DMA((Z, S - 1)), DMA((Z, S)), DMA((S, Z)), DMA((S, Z)), DMA((Z,)), DMA((Z,)),
        DMA((S,)), DMA((S,)), DMA((T,)), DMA((T,)),
    ]
    return pl.pallas_call(
        kernel,
        out_shape=jax.ShapeDtypeStruct(latent.shape, bf16),
        in_specs=[VM] * 4 + [ANY] * 11,
        out_specs=VM,
        scratch_shapes=scratch,
        compiler_params=pltpu.CompilerParams(
            collective_id=1, has_side_effects=True, vmem_limit_bytes=60 * 1024 * 1024
        ),
    )(*args)


def solution(mesh):
    in_specs = (
        P(("sp", "tp"), None),
        P("sp", None),
        P(),
        P(),
        P(None, "sp", "tp"),
        P(),
        P("tp", None),
        P("tp", None),
        P(),
        P(),
        P(),
        P(None, "tp"),
        P(None, "tp"),
        P(None, "tp"),
        P(),
        P(),
        P("tp"),
        P("tp", None),
    )
    out_specs = P(("sp", "tp"), None)
    return jax.shard_map(shards, mesh=mesh, in_specs=in_specs, out_specs=out_specs, check_vma=False)
```

```python
import math

import jax
import jax.numpy as jnp
import numpy as np
from jax import lax
from jax.experimental import pallas as pl
from jax.experimental.pallas import tpu as pltpu
from jax.sharding import PartitionSpec as P

NOPE = 64
ROPE = 32
VDIM = 64
GRID_W = 64
TOK_DEV = 1024
CTX_DEV = 32
CORES = 2
KD = NOPE + ROPE
WIDE = KD + VDIM

epsilon = 1e-06
theta = 10000.0

NT = (((1,), (1,)), ((), ()))
TN = (((0,), (0,)), ((), ()))
TT = (((0,), (1,)), ((), ()))


def axial_tables(count):
    pair_count = ROPE // 4
    positions = np.arange(count)
    frequency = np.power(theta, -np.arange(pair_count, dtype=np.float32) / pair_count).astype(np.float32)
    row_angle = (positions // GRID_W).astype(np.float32)[None, :] * frequency[:, None]
    col_angle = (positions % GRID_W).astype(np.float32)[None, :] * frequency[:, None]
    tables = [np.cos(row_angle), np.sin(row_angle), np.cos(col_angle), np.sin(col_angle)]
    return np.stack(tables).astype(np.float32)


def remote(source, target, send, recv, device):
    return pltpu.make_async_remote_copy(
        src_ref=source,
        dst_ref=target,
        send_sem=send,
        recv_sem=recv,
        device_id=device,
        device_id_type=pl.DeviceIdType.MESH,
    )


def loop(low, high, body):
    def step(k, carry):
        body(k)
        return carry

    lax.fori_loop(low, high, step, 0)


class Here:
    def __init__(self):
        self.sp, self.tp = lax.axis_index("sp"), lax.axis_index("tp")
        self.S, self.T = lax.axis_size("sp"), lax.axis_size("tp")
        self.X = math.isqrt(self.S)
        assert self.X * self.X == self.S
        self.y, self.x = self.sp // self.X, lax.rem(self.sp, self.X)
        self.Z = self.T // CORES
        self.z, self.core = self.tp // CORES, lax.rem(self.tp, CORES)
        self.mate = {"tp": self.tp + 1 - 2 * self.core}

    def greet(self):
        barrier = pltpu.get_barrier_semaphore()
        for k in range(1, self.S):
            to = lax.rem(self.sp + k, self.S)
            pl.semaphore_signal(barrier, inc=1, device_id={"sp": to}, device_id_type=pl.DeviceIdType.MESH)
        for k in range(1, self.T):
            to = lax.rem(self.tp + k, self.T)
            pl.semaphore_signal(barrier, inc=1, device_id={"tp": to}, device_id_type=pl.DeviceIdType.MESH)
        pl.semaphore_wait(barrier, self.S + self.T - 2)

    def block(self, r):
        z, Z = self.z, self.Z
        near = lax.min(z, Z - 1 - z)
        zig = ((r + 1) // 2) * (2 * lax.rem(r, 2) - 1)
        far = (r - near) * jnp.where(z <= Z - 1 - z, 1, -1)
        return z + jnp.where(r <= 2 * near, zig, far)

    def part(self, dy, dx):
        X = self.X
        return lax.rem(self.y + dy + X, X) * X + lax.rem(self.x + dx + X, X)


class Line:
    def __init__(self, at, own, slot, send, recv):
        self.at, self.own, self.slot, self.send, self.recv = at, own, slot, send, recv

    def hop(self, block, step, first=False):
        at = self.at
        to = lax.max(lax.min(at.z + step, at.Z - 1), 0)
        return remote(
            self.own if first else self.slot(block),
            self.slot(block),
            self.send.at[block, (1 - step) // 2],
            self.recv.at[block],
            {"tp": to * CORES + at.core},
        )

    def ends(self, step):
        return (self.at.z + step >= 0) & (self.at.z + step < self.at.Z)

    def start(self):
        for step in (1, -1):

            @pl.when(self.ends(step))
            def _():
                self.hop(self.at.z, step, True).start()

    def way(self, block):
        return jnp.where(block < self.at.z, 1, -1)

    def arrive(self, block):
        step = self.way(block)
        self.hop(block, step).wait_recv()

        @pl.when(self.ends(step))
        def _():
            self.hop(block, step).start()

    def drain(self):
        for step in (1, -1):

            @pl.when(self.ends(step))
            def _():
                self.hop(self.at.z, step, True).wait_send()

        def body(r):
            block = self.at.block(r)
            step = self.way(block)

            @pl.when(self.ends(step))
            def _():
                self.hop(block, step).wait_send()

        loop(1, self.at.Z, body)


class Direct(Line):
    def hop(self, block, to):
        at = self.at
        return remote(self.own, self.slot(block), self.send.at[to, 0], self.recv.at[block], {"tp": to * CORES + at.core})

    def start(self):
        loop(1, self.at.Z, lambda r: self.hop(self.at.z, self.at.block(r)).start())

    def arrive(self, block):
        self.hop(block, self.at.z).wait_recv()

    def drain(self):
        loop(1, self.at.Z, lambda r: self.hop(self.at.z, self.at.block(r)).wait_send())


class Plane:
    def __init__(self, at, slot, send, recv):
        self.at, self.slot, self.send, self.recv = at, slot, send, recv

    def side(self, b):
        return lax.rem(b + self.at.core, 2)

    def place(self, e, i, j):
        return self.at.part(i * e + j * (1 - e), i * (1 - e) + j * e)

    def copy(self, b, s, to, sem):
        return remote(self.slot(b, s), self.slot(b, s), self.send.at[b, sem], self.recv.at[b, s], {"sp": to})

    def sends(self, b, first, second, act):
        X, e = self.at.X, self.side(b)
        if first:
            for i in range(1, X):
                act(self.copy(b, self.at.sp, self.place(e, i, 0), i - 1))
            for j in range(1, X):
                act(self.copy(b, self.at.sp, self.place(e, 0, j), X + j - 2))
        if second:
            for i in range(1, X):
                for j in range(1, X):
                    sem = 2 * (X - 1) + (i - 1) * (X - 1) + j - 1
                    act(self.copy(b, self.place(e, -i, 0), self.place(e, 0, j), sem))

    def push(self, b):
        self.sends(b, True, False, lambda copy: copy.start())

    def take(self, b, s):
        self.copy(b, s, self.place(0, 1, 0), 0).wait_recv()

    def forward(self, b, then=None):
        e = self.side(b)
        for i in range(1, self.at.X):
            s = self.place(e, -i, 0)
            self.take(b, s)
            if then is not None:
                then(b, s)
        self.sends(b, False, True, lambda copy: copy.start())

    def rest(self, b):
        e = self.side(b)
        for j in range(1, self.at.X):
            for i in range(self.at.X):
                self.take(b, self.place(e, -i, -j))

    def drain(self, b):
        self.sends(b, True, True, lambda copy: copy.wait_send())


class Mate:
    def __init__(self, at, slot, send, recv):
        self.at, self.slot, self.send, self.recv = at, slot, send, recv

    def copy(self, core, *key):
        return remote(self.slot(core, *key), self.slot(core, *key), self.send.at[key], self.recv.at[key], self.at.mate)

    def give(self, *key):
        self.copy(self.at.core, *key).start()

    def take(self, *key):
        self.copy(1 - self.at.core, *key).wait_recv()

    def drain(self, *key):
        self.copy(self.at.core, *key).wait_send()


def rms(tensor, axis):
    return tensor * lax.rsqrt(jnp.mean(tensor * tensor, axis=axis, keepdims=True) + epsilon)


def kernel(
    cond_in, cond_context_in, gain_in, qlat_in, kvlat_in, gain_q_in, gain_k_in, bias_in,
    latent, context, mod_weight, dq, dkv, ow, rope_t, uq_t_in, uk, uv, tables_in,
    out,
    cond, cond_context, norm_gain, qlat_gain, kvlat_gain, gain_row, bias,
    lat, con, mw, rope, uq_t, up_k, up_v, tables, uk_t, gains,
    dq_all, dkv_all, ow_all, pm, msum, mods, normed,
    kv_lats, q_lats, ctx_lats, q, keys, values, ctx_kv, ctx_values, m_scr, acc, att, att_in,
    local, p_send, p_recv, t_send, t_recv,
    wl_send, wl_recv, wp_send, wp_recv, wm_send, wm_recv,
    ll_send, ll_recv, lp_send, lp_recv, lm_send, lm_recv, qm_send, qm_recv,
    x_send, x_recv, a_send, a_recv,
):
    at = Here()
    sp, tp, S, T, Z, z, core = at.sp, at.tp, at.S, at.T, at.Z, at.z, at.core
    f32, bf16 = jnp.float32, jnp.bfloat16
    H, N, _ = q.shape
    rows = out.shape[0]
    span = rows * CORES
    ctx_rows = con.shape[0]
    width = latent.shape[1]
    G = 2 if Z % 2 == 0 else 1
    TQ = span * G
    LAG = 2
    tiles = Z // G
    factor = KD ** (-0.5) * math.log2(math.e)

    loads = [
        pltpu.make_async_copy(a, b, local.at[i])
        for i, (a, b) in enumerate((
            (mod_weight, mw), (cond_in, cond), (cond_context_in, cond_context),
            (latent, lat), (context, con), (gain_in, norm_gain),
            (uq_t_in, uq_t), (uk, up_k), (uv, up_v), (rope_t, rope), (qlat_in, qlat_gain), (kvlat_in, kvlat_gain),
            (gain_q_in, gain_row.at[0]), (gain_k_in, gain_row.at[1]), (bias_in, bias), (tables_in, tables),
            (dq, dq_all.at[z, core]), (dkv, dkv_all.at[z, core]), (ow, ow_all.at[z, core]),
        ))
    ]
    for copy in loads:
        copy.start()
    at.greet()

    weights = ((dkv, dkv_all), (dq, dq_all), (ow, ow_all))
    w_lines, w_planes, w_mates = [], [], []
    for i, (own, every) in enumerate(weights):
        w_lines.append((Direct if i == 0 else Line)(
            at, own.at[sp], (lambda e: lambda b: e.at[b, core, sp])(every), wl_send.at[i], wl_recv.at[i]
        ))
        w_planes.append(Plane(at, (lambda e: lambda b, s: e.at[b, core, s])(every), wp_send.at[i], wp_recv.at[i]))
        w_mates.append(Mate(at, (lambda e: lambda c, b: e.at[b, c])(every), wm_send.at[i], wm_recv.at[i]))

    def own_mate(i):
        own, every = weights[i]
        return remote(own, every.at[z, core], wm_send.at[i, z], wm_recv.at[i, z], at.mate)

    for i in range(2):
        w_lines[i].start()

    span_k = mw.shape[1]

    def silu(v):
        return v / (1.0 + jnp.exp(-v))

    def row(ref):
        block = ref[...].astype(f32)
        return jnp.concatenate([block[i : i + 1, :] for i in range(block.shape[0])], axis=1)

    for copy in loads[:3]:
        copy.wait()
    wide = []
    for ref in (cond, cond_context):
        every = row(ref)
        mine = every[:, :span_k]
        for i in range(1, S):
            mine = jnp.where(sp == i, every[:, i * span_k : (i + 1) * span_k], mine)
        wide.append(jnp.broadcast_to(silu(mine), (8, span_k)))
    index = lax.broadcasted_iota(jnp.int32, (8, span_k), 0)
    part = jnp.zeros(pm.shape[1:], f32)
    for r in range(mw.shape[0]):
        act = jnp.where(index == 2 * r, wide[0], jnp.where(index == 2 * r + 1, wide[1], 0.0)).astype(bf16)
        part = part + jnp.dot(act, mw[r], preferred_element_type=f32)
    pm[sp] = part

    def part_copy(k):
        return remote(pm.at[sp], pm.at[sp], p_send.at[k], p_recv.at[k], {"sp": lax.rem(sp + k, S)})

    def part_wait(k):
        to = pm.at[lax.rem(sp - k + S, S)]
        remote(to, to, p_send.at[k], p_recv.at[k], {"sp": lax.rem(sp + k, S)}).wait_recv()

    def mod_copy(k):
        return remote(msum, mods.at[tp], t_send.at[k], t_recv.at[k], {"tp": lax.rem(tp + k, T)})

    def mod_wait(k):
        to = mods.at[lax.rem(tp - k + T, T)]
        remote(to, to, t_send.at[k], t_recv.at[k], {"tp": lax.rem(tp + k, T)}).wait_recv()

    loop(1, S, lambda k: part_copy(k).start())
    for i in range(2):
        own_mate(i).start()
    loop(1, S, part_wait)
    total = pm[0]
    for k in range(1, S):
        total = total + pm[k]
    msum[...] = total
    mods[tp] = total
    loop(1, T, lambda k: mod_copy(k).start())

    def weights_arrive(r):
        b = at.block(r)
        for i in range(2):
            w_lines[i].arrive(b)
            w_planes[i].push(b)

    def weights_forward(r):
        b = at.block(r)
        for i in range(2):
            w_planes[i].forward(b)

    for r in range(1, Z):
        weights_arrive(r)
        if r > 1:
            weights_forward(r - 1)
    w_lines[2].start()
    weights_forward(Z - 1)

    for copy in loads[3:16]:
        copy.wait()
    uk_t[...] = up_k[...].astype(f32).T.astype(bf16)
    for i in range(2):
        line = jnp.concatenate([gain_row[i], jnp.zeros((1, 128 - KD), f32)], axis=1)
        gains[i] = jnp.broadcast_to(line, (128, 128)).T[:KD, :]
    shift = [(bias[:, h : h + 1] + math.log(TOK_DEV / CTX_DEV)) * math.log2(math.e) for h in range(H)]

    loop(1, T, mod_wait)
    gain = row(norm_gain)
    every_mod = jnp.concatenate([mods[t] for t in range(T)], axis=1)

    def modulate(source, count, base, kind):
        step = math.gcd(count, 32)
        for i in range(count // step):
            u = source[i * step : (i + 1) * step, :].astype(f32)
            u = rms(u, 1) * gain * (1.0 + every_mod[2 + kind : 3 + kind, :]) + every_mod[kind : kind + 1, :]
            normed[base + i * step : base + (i + 1) * step, :] = u.astype(bf16)

    modulate(lat, rows, 0, 0)
    modulate(con, ctx_rows, rows, 1)

    def gather_rest(i):
        for r in range(1, Z):
            b = at.block(r)
            w_planes[i].rest(b)
            w_mates[i].give(b)
        for b in range(Z):
            w_mates[i].take(b)

    gather_rest(0)
    for copy in loads[16:]:
        copy.wait()

    def put_tail(ref, t):
        base, count = ref.shape[0] - 16, t.shape[1]
        ref[base:, 0:count] = t[:16, :]
        ref[base:, 128 : 128 + count] = t[16:, :]

    def get_tail(block, count):
        return jnp.concatenate([block[-16:, 0:128], block[-16:, 128:256]], axis=0)[:, :count]

    stacked = normed[...]
    kv_down = jnp.dot(stacked, dkv_all[...].reshape(width, -1), preferred_element_type=f32)
    kv_latent = (rms(kv_down, 1) * row(kvlat_gain)).astype(bf16)
    rope_rows = lax.dot_general(rope[...], stacked, NT, preferred_element_type=f32).astype(bf16)
    own_kv = kv_lats.at[sp, z, core]
    own_kv[:rows, :] = kv_latent[:rows]
    put_tail(own_kv, rope_rows[:, :rows])
    own_ctx = ctx_lats.at[sp]
    own_ctx[:ctx_rows, :] = kv_latent[rows:]
    put_tail(own_ctx, rope_rows[:, rows:])

    kv_line = Line(at, own_kv, lambda b: kv_lats.at[sp, b, core], ll_send.at[0], ll_recv.at[0])
    kv_plane = Plane(at, lambda b, s: kv_lats.at[s, b, core], lp_send, lp_recv)
    kv_mate = Mate(at, lambda c, s, b: kv_lats.at[s, b, c], lm_send, lm_recv)
    q_line = Line(at, q_lats.at[z, core], lambda b: q_lats.at[b, core], ll_send.at[1], ll_recv.at[1])
    q_mate = Mate(at, lambda c, b: q_lats.at[b, c], qm_send, qm_recv)

    kv_line.start()
    kv_plane.push(z)
    kv_mate.give(sp, z)

    def ctx_copy(k):
        return remote(own_ctx, own_ctx, x_send.at[k], x_recv.at[k], {"sp": lax.rem(sp + k, S)})

    def ctx_wait(k):
        to = ctx_lats.at[lax.rem(sp - k + S, S)]
        remote(to, to, x_send.at[k], x_recv.at[k], {"sp": lax.rem(sp + k, S)}).wait_recv()

    loop(1, S, lambda k: ctx_copy(k).start())

    gather_rest(1)
    query_down = jnp.dot(normed[:rows, :], dq_all[...].reshape(width, -1), preferred_element_type=f32)
    q_lats[z, core] = (rms(query_down, 1) * row(qlat_gain)).astype(bf16)
    q_line.start()
    q_mate.give(z)

    def turned(u, gain, where):
        u = rms(u, 0) * gain[:, :1]
        if where is None:
            return u
        m = ROPE // 4
        a, b, c, d = (u[NOPE + i * m : NOPE + (i + 1) * m, :] for i in range(4))
        rc, rs, cc, cs = (tables[i, :, where] for i in range(4))
        return jnp.concatenate(
            [u[:NOPE, :], a * rc - b * rs, b * rc + a * rs, c * cc - d * cs, d * cc + c * cs], axis=0
        )

    def expand_keys(rows_in, tail_in, put, where):
        u = lax.dot_general(uk_t[...], rows_in, NT, preferred_element_type=f32)
        for h in range(H):
            key = jnp.concatenate([u[h * NOPE : (h + 1) * NOPE, :], tail_in.astype(f32)], axis=0)
            put(h, turned(key, gains[1], where).astype(bf16))

    def expand_values(rows_in, put):
        u = jnp.dot(rows_in, up_v[...], preferred_element_type=f32).astype(bf16)
        ones = jnp.ones((rows_in.shape[0], 128 - VDIM), bf16)
        for h in range(H):
            put(h, jnp.concatenate([u[:, h * VDIM : (h + 1) * VDIM], ones], axis=1))

    def joined(blocks, count):
        return (
            jnp.concatenate([block[:count, :] for block in blocks], axis=0),
            jnp.concatenate([get_tail(block, count) for block in blocks], axis=1),
        )

    def kv_arrive(r):
        b = at.block(r)
        kv_line.arrive(b)
        kv_plane.push(b)
        kv_mate.give(sp, b)

    def kv_forward(r):
        kv_plane.forward(at.block(r), lambda b, s: kv_mate.give(s, b))

    def kv_rest(r):
        b = at.block(r)
        e = kv_plane.side(b)
        for j in range(1, at.X):
            for i in range(at.X):
                s = kv_plane.place(e, -i, -j)
                kv_plane.take(b, s)
                kv_mate.give(s, b)

    def chunk_expand(c):
        b = at.block(c)

        def body(s):
            kv_mate.take(s, b)
            rows_in, tail_in = joined([kv_lats[s, b, i] for i in range(CORES)], rows)
            here = pl.ds(pl.multiple_of(s * span, span), span)

            def put_key(h, key):
                keys[c, h, :, here] = key

            def put_value(h, value):
                values[c, h, here, :] = value

            expand_keys(rows_in, tail_in, put_key, pl.ds(pl.multiple_of(s * N + b * span, span), span))
            expand_values(rows_in, put_value)

        loop(0, S, body)

    def q_arrive(r):
        b = at.block(r)
        q_line.arrive(b)
        q_mate.give(b)

    def tile_at(t):
        return pl.ds(pl.multiple_of(t * TQ, TQ), TQ)

    def absorb(where, kts, vts, shifts, first):
        scores = [jnp.dot(q[h, where, :][:, :KD], kts[h], preferred_element_type=f32) for h in range(H)]
        olds = [None if first else m_scr[h, where, :][:, :1] for h in range(H)]
        accs = [None if first else acc[h, where, :] for h in range(H)]
        news, sums = [], []
        for h in range(H):
            s = scores[h]
            new = jnp.max(s, axis=1, keepdims=True) * factor
            if shifts is not None:
                new = new + shifts[h]
            base = new
            if not first:
                new = jnp.maximum(olds[h], new)
            base = new if shifts is None else new - shifts[h]
            p = jnp.exp2(s * factor - base)
            o = jnp.dot(p.astype(bf16), vts[h], preferred_element_type=f32)
            news.append(new)
            sums.append(o if first else accs[h] * jnp.exp2(olds[h] - new) + o)
        for h in range(H):
            m_scr[h, where, :] = jnp.broadcast_to(news[h], (TQ, 128))
            acc[h, where, :] = sums[h]

    def tile_expand(t):
        for g in range(G):
            b = at.block(t * G + g)
            q_mate.take(b)
            rows_in = q_lats[b].reshape(span, q_lats.shape[3])
            u = lax.dot_general(uq_t[...], rows_in, NT, preferred_element_type=f32)
            spot = pl.ds(pl.multiple_of(sp * N + b * span, span), span)
            where = pl.ds(pl.multiple_of(t * TQ + g * span, span), span)
            for h in range(H):
                query = turned(u[h * KD : (h + 1) * KD, :], gains[0], spot)
                query = jnp.concatenate([query, jnp.zeros((128 - KD, span), f32)], axis=0)
                q[h, where, :] = query.T.astype(bf16)
        absorb(
            tile_at(t), [ctx_kv[h, :KD, :] for h in range(H)],
            [ctx_values[h] for h in range(H)], shift, True,
        )

    def pair(t, c):
        absorb(tile_at(t), [keys[c, h] for h in range(H)], [values[c, h] for h in range(H)], None, False)

    def owner_rows(r, i):
        return att.at[pl.ds(pl.multiple_of(r * span + i * rows, rows), rows)]

    def give(r, i):
        dest = at.block(r) * CORES + i
        return remote(owner_rows(r, i), att_in.at[tp], a_send.at[dest], a_recv.at[tp], {"tp": dest})

    def finish(t):
        where = tile_at(t)
        parts = [acc[h, where, :] for h in range(H)]
        heads = [part[:, :VDIM] / part[:, VDIM : 2 * VDIM] for part in parts]
        att[where, :] = jnp.concatenate(heads, axis=1).astype(bf16)
        for g in range(G):
            r = t * G + g
            for i in range(CORES):

                @pl.when((at.block(r) != z) | (core != i))
                def _():
                    give(r, i).start()

                @pl.when((at.block(r) == z) & (core == i))
                def _():
                    att_in[tp] = owner_rows(r, i)[...]

    for r in range(1, 3):
        if r < Z:
            w_lines[2].arrive(at.block(r))
            kv_arrive(r)
        if r - 1 < Z:
            kv_forward(r - 1)
        if r >= 2:
            kv_rest(r - 2)
    own_mate(2).start()

    loop(1, S, ctx_wait)
    rows_in, tail_in = joined([ctx_lats[s] for s in range(S)], ctx_rows)

    def put_ctx_key(h, key):
        ctx_kv[h, :KD, :] = key

    def put_ctx_value(h, value):
        ctx_values[h] = value

    expand_keys(rows_in, tail_in, put_ctx_key, None)
    expand_values(rows_in, put_ctx_value)

    steps = Z + LAG * (tiles - 1)

    def step(w):
        k = w + 3

        @pl.when(w + 1 < Z)
        def _():
            q_arrive(w + 1)

        @pl.when(k < Z)
        def _():
            w_lines[2].arrive(at.block(k))
            kv_arrive(k)

        @pl.when(k - 1 < Z)
        def _():
            kv_forward(k - 1)

        @pl.when(k - 1 == Z - 1)
        def _():
            loop(1, Z, lambda r: w_planes[2].push(at.block(r)))

        @pl.when(k - 2 < Z)
        def _():
            kv_rest(k - 2)

        @pl.when(k - 2 == Z)
        def _():
            loop(1, Z, lambda r: w_planes[2].forward(at.block(r)))

        @pl.when(w < Z)
        def _():
            chunk_expand(w)

        for t in range(tiles):
            c = w - LAG * t

            @pl.when(c == 0)
            def _():
                tile_expand(t)

            @pl.when((c >= 0) & (c < Z))
            def _():
                pair(t, c)

            @pl.when(c == Z - 1)
            def _():
                finish(t)

    loop(0, steps, step)

    def ow_rest(r):
        b = at.block(r)
        w_planes[2].rest(b)
        w_mates[2].give(b)

    loop(1, Z, ow_rest)
    loop(0, Z, lambda b: w_mates[2].take(b))

    def att_wait(k):
        source = lax.rem(tp - k + T, T)
        to = att_in.at[source]
        remote(to, to, a_send.at[source], a_recv.at[source], {"tp": source}).wait_recv()

    loop(1, T, att_wait)
    attended = jnp.concatenate([att_in[t] for t in range(T)], axis=1)
    cut = mods.shape[2]
    for t in range(T):
        where = slice(t * cut, (t + 1) * cut)
        weight = ow_all[:, :, :, :, where].reshape(-1, cut)
        projected = jnp.dot(attended, weight, preferred_element_type=f32)
        out[:, where] = (lat[:, where].astype(f32) + mods[t, 4:5, :] * projected).astype(bf16)

    loop(1, S, lambda k: part_copy(k).wait_send())
    loop(1, T, lambda k: mod_copy(k).wait_send())
    loop(1, S, lambda k: ctx_copy(k).wait_send())
    for r in range(Z):
        for i in range(CORES):

            @pl.when((r > 0) | (core != i))
            def _():
                give(r, i).wait_send()

    for i in range(3):
        own_mate(i).wait_send()
        w_lines[i].drain()

        def body(r):
            w_planes[i].drain(at.block(r))
            w_mates[i].drain(at.block(r))

        loop(1, Z, body)
    kv_line.drain()
    q_line.drain()

    def body(b):
        kv_plane.drain(b)
        q_mate.drain(b)
        loop(0, S, lambda s: kv_mate.drain(s, b))

    loop(0, Z, body)


DMA = pltpu.SemaphoreType.DMA
VM = pl.BlockSpec(memory_space=pltpu.VMEM)
ANY = pl.BlockSpec(memory_space=pl.ANY)


def shards(
    latent, context, cond, cond_context, mod_weight, norm_gain, down_q, down_kv, rope_weight, qlat_gain, kvlat_gain,
    up_query, up_key, up_value, query_gain, key_gain, context_bias, out_weight,
):
    S, T = lax.axis_size("sp"), lax.axis_size("tp")
    Z = T // CORES
    bf16, f32 = jnp.bfloat16, jnp.float32
    own_rows, width = latent.shape
    ctx_rows = context.shape[0]
    N = own_rows * T
    cols = mod_weight.shape[2]
    dq, dkv, ow = (w.reshape(S, w.shape[0] // S, w.shape[1]) for w in (down_q, down_kv, out_weight))
    QR, KR = down_q.shape[1], down_kv.shape[1]
    H = up_key.shape[1] // NOPE

    def lines(v):
        return v.reshape(-1, 128)

    tables = jnp.asarray(axial_tables(S * N))
    small = [lines(v) for v in (cond, cond_context, norm_gain, qlat_gain, kvlat_gain)]
    small += [query_gain[None, :], key_gain[None, :], context_bias[None, :]]
    args = small + [
        latent, context, mod_weight, dq, dkv, ow, rope_weight.T, up_query.T, up_key, up_value, tables,
    ]
    lat_rows, span = own_rows + 16, own_rows * CORES
    V = pltpu.VMEM
    scratch = [V(v.shape, v.dtype) for v in small[:5]]
    scratch += [
        V((2, 1, KD), f32), V((1, H), f32),
        V(latent.shape, bf16), V(context.shape, bf16), V(mod_weight.shape, bf16), V(rope_weight.shape[::-1], bf16),
        V(up_query.shape[::-1], bf16), V(up_key.shape, bf16), V(up_value.shape, bf16), V(tables.shape, f32),
        V(up_key.shape[::-1], bf16), V((2, KD, 128), f32),
        V((Z, CORES) + dq.shape, bf16), V((Z, CORES) + dkv.shape, bf16), V((Z, CORES) + ow.shape, bf16),
        V((S, 8, cols), f32), V((8, cols), f32), V((T, 8, cols), f32), V((own_rows + ctx_rows, width), bf16),
        V((S, Z, CORES, lat_rows, KR), bf16), V((Z, CORES, own_rows, QR), bf16), V((S, ctx_rows + 16, KR), bf16),
        V((H, N, 128), bf16), V((Z, H, KD, S * span), bf16), V((Z, H, S * span, 128), bf16),
        V((H, KD, S * ctx_rows), bf16), V((H, S * ctx_rows, 128), bf16),
        V((H, N, 128), f32), V((H, N, 128), f32),
        V((N, H * VDIM), bf16), V((T, own_rows, H * VDIM), bf16),
        DMA((19,)), DMA((S,)), DMA((S,)), DMA((T,)), DMA((T,)),
        DMA((3, Z, 2)), DMA((3, Z)), DMA((3, Z, S - 1)), DMA((3, Z, S)), DMA((3, Z)), DMA((3, Z)),
        DMA((2, Z, 2)), DMA((2, Z)), DMA((Z, S - 1)), DMA((Z, S)), DMA((S, Z)), DMA((S, Z)), DMA((Z,)), DMA((Z,)),
        DMA((S,)), DMA((S,)), DMA((T,)), DMA((T,)),
    ]
    return pl.pallas_call(
        kernel,
        out_shape=jax.ShapeDtypeStruct(latent.shape, bf16),
        in_specs=[ANY] * len(args),
        out_specs=VM,
        scratch_shapes=scratch,
        compiler_params=pltpu.CompilerParams(
            collective_id=1, has_side_effects=True, vmem_limit_bytes=60 * 1024 * 1024
        ),
    )(*args)


def solution(mesh):
    in_specs = (
        P(("sp", "tp"), None),
        P("sp", None),
        P(),
        P(),
        P(None, "sp", "tp"),
        P(),
        P("tp", None),
        P("tp", None),
        P(),
        P(),
        P(),
        P(None, "tp"),
        P(None, "tp"),
        P(None, "tp"),
        P(),
        P(),
        P("tp"),
        P("tp", None),
    )
    out_specs = P(("sp", "tp"), None)
    return jax.shard_map(shards, mesh=mesh, in_specs=in_specs, out_specs=out_specs, check_vma=False)
```
